32 devices in a mesh: sp: 16 (over z, y, x), tp: 2 (over core).
Axes of the slice: x: 2, y: 2, z: 4, core: 2. Of those that a mesh axis runs over, the one named last changes fastest.
Arguments:
- moe_input: bfloat16 [2048, 2048], P('sp'), may hold values from -6 to 6
- out_grad: bfloat16 [2048, 2048], P('sp'), may hold values from -8 to 8
- route_ids: int32 [2048, 2], P('sp'), may hold values from 0 to 7, all different within a row; in each aligned block of 128 rows (0 to 127, 128 to 255, ...) at most 48 rows name the same one
- route_weights: float32 [2048, 2], P('sp'), may hold values from 0.1 to 0.9
- gate_w: bfloat16 [16, 2048, 1792], P('sp', None, 'tp'), may hold values from -0.125 to 0.125
- up_w: bfloat16 [16, 2048, 1792], P('sp', None, 'tp'), may hold values from -0.125 to 0.125
- down_w: bfloat16 [16, 1792, 2048], P('sp', 'tp'), may hold values from -0.09375 to 0.09375
- mixer_out: bfloat16 [2048, 1024], P('sp', 'tp'), may hold values from -6 to 6
- out_weight: bfloat16 [1024, 2048], P('tp'), may hold values from -0.1875 to 0.1875
- queries: bfloat16 [2048, 512], P('sp', 'tp'), may hold values from -0.125 to 0.125
- keys: bfloat16 [2048, 512], P('sp', 'tp'), may hold values from -0.3125 to 0.3125
- values: bfloat16 [2048, 1024], P('sp', 'tp'), may hold values from -1.5 to 1.5
- log_decay: float32 [2048, 512], P('sp', 'tp'), may hold values from -0.1 to 0, as said below
- block_states: float32 [32, 8, 64, 128], P('sp', 'tp'), may hold values from -1.75 to 1.75
Outputs:
- grad_queries: bfloat16 [2048, 512], P('sp', 'tp')
- grad_keys: bfloat16 [2048, 512], P('sp', 'tp')
- grad_values: bfloat16 [2048, 1024], P('sp', 'tp')
- grad_decay: float32 [2048, 512], P('sp', 'tp')
- grad_out_weight: float32 [1024, 2048], P('tp', 'sp')
- grad_gate_w: bfloat16 [16, 2048, 1792], P('sp', None, 'tp')
- grad_up_w: bfloat16 [16, 2048, 1792], P('sp', None, 'tp')
- grad_down_w: bfloat16 [16, 1792, 2048], P('sp', 'tp')
The draws below stay inside these ranges and needn't reach their ends.
Inputs may be any that keep to these rules, and one draw needn't show every extreme that they name: `route_ids`: each row names two different experts. In the rows of one index of sp no expert is named more than 48 times, and in every draw some expert is named exactly 48 times by the rows of some index of sp. `log_decay`: Negative.
All inputs are finite; a program needn't handle non-finite values.
Results may differ from the reference program's by a relative error of at most 0.013.
Values may be sent and summed in bfloat16 or wider, within the bound.
A program may use at most 128 MiB of HBM per device.

```python
import math
import jax
import jax.numpy as jnp
import numpy as np
from jax import lax

D = 2048
HEADS = 8
DK = 64
DV = 128
FFE = 3584
BLK = 64
TOK_DEV = 128
TOKENS = 2048
HK = 512
HV = 1024
NBLK = 32
EXPERTS = 8
FH = 1792
FQ = 896
CAP = 48
SLOTS = 768
N_SP = 16
N_TP = 2


def draw_log_decay(key, part):
    key_kind, key_block, key_rough = jax.random.split(key, 3)
    channels = HEADS * DK
    slow_share = 5
    slow_channel = jax.random.randint(key_kind, (channels,), 0, 10) < slow_share
    base_rate = jnp.where(slow_channel, 2.0 / TOKENS, 1.0 / 40.0).astype(jnp.float32)
    factor = jnp.exp(jax.random.uniform(key_block, (TOKENS // TOK_DEV,), jnp.float32, jnp.log(0.4), jnp.log(2.5)))
    roughness = jax.random.uniform(key_rough, (TOKENS, channels), jnp.float32, 0.5, 1.5)
    per_token = jnp.repeat(factor, TOK_DEV)
    return (-(base_rate[None, :] * per_token[:, None] * roughness)).astype(jnp.float32)


def with_spikes(entries, rng, source, target, shards_of, factor):
    def block_of(axis_at):
        return (jnp.arange(entries.shape[axis_at]) // (entries.shape[axis_at] // shards_of)).reshape((-1,) + (1,) * (entries.ndim - 1 - axis_at))

    first = jax.random.permutation(rng, shards_of)[block_of(target)]
    far = (block_of(target) + shards_of // 2) % shards_of
    return jnp.where((block_of(source) == first) | (block_of(source) == far), factor * entries, entries)


def block_levels(stream_key, dims, cuts, low, top_value):
    factor_of, own = 1.0, jax.random.fold_in(stream_key, 6)
    for dim, shards_of in cuts:
        draws = jnp.exp(jax.random.uniform(jax.random.fold_in(own, dim), (shards_of,), jnp.float32, low / len(cuts), top_value / len(cuts)))
        factor_of = factor_of * jnp.repeat(draws, dims[dim] // shards_of).reshape([-1 if axis == dim else 1 for axis in range(len(dims))])
    return factor_of


def deal_out(own_key, own, number, rows, number_of, top, bound, lean):
    sequence = jax.random.permutation(own_key, number_of)
    packed, common = portions_of(number_of, rows * top, bound, lean, True), portions_of(number_of, rows * top, bound, lean, False)
    places = jnp.arange(number_of)

    def named(lengths, rotation):
        used = int((lengths > 0).sum())
        fixed = max(1, used // 4)
        passed = fixed + (places - fixed + rotation * (used - fixed)) % max(1, number_of - fixed)
        return jnp.zeros((number_of,), jnp.int32).at[sequence[jnp.where(places < fixed, places, passed)]].set(jnp.asarray(lengths, jnp.int32))

    lengths = jnp.where(number % 4 == 0, named(packed, number // 4), named(common, number - number // 4 - 1))
    mixed = jax.random.permutation(jax.random.fold_in(own, 3), number_of)
    donor, taker = mixed[0:number_of // 2 * 2:2], mixed[1:number_of // 2 * 2:2]
    margin = jnp.minimum(lengths[donor] - 1, bound - lengths[taker]) // 2
    margin = jnp.where((donor == sequence[0]) | (taker == sequence[0]) | (lengths[taker] == 0), 0, jnp.maximum(margin, 0))
    passed = jax.random.randint(jax.random.fold_in(own, 4), (number_of // 2,), 0, 1 << 20) % (margin + 1)
    lengths = lengths.at[donor].add(-passed).at[taker].add(passed)
    items = jnp.searchsorted(jnp.cumsum(lengths), jnp.arange(rows * top), side="right").astype(jnp.int32)
    table = items.reshape(top, rows).T
    table = table[jax.random.permutation(jax.random.fold_in(own, 1), rows)]
    rotation = jax.random.randint(jax.random.fold_in(own, 2), (rows, 1), 0, top)
    return jnp.take_along_axis(table, (jnp.arange(top)[None, :] + rotation) % top, axis=1)


def portions_of(count, total, bound, lean, full):
    weights = [(1 << 20) // math.isqrt(rank ** lean) + 1 for rank in range(1, count + 1)]
    largest = bound if full else min(bound, max(-(-total // count), total * weights[0] // sum(weights)))
    least = 1 if total - largest >= count - 1 else 0
    counts, rest = [largest] + [least] * (count - 1), total - largest - least * (count - 1)
    while rest > 0:
        candidates = [i for i in range(1, count) if counts[i] < largest] or [i for i in range(1, count) if counts[i] < bound]
        pool, remaining = sum([weights[i] for i in candidates]), rest
        for i in candidates:
            more = min(bound - counts[i], max(1, remaining * weights[i] // pool), rest)
            counts[i] = counts[i] + more
            rest = rest - more
    return np.array(counts)


def scatter_about(stream_key, shape, deviation, most, shards=(), kind=jnp.bfloat16):
    factor_of = block_levels(stream_key, shape, shards, -0.22, 0.18) if shards else 1.0
    drawn = jax.random.normal(stream_key, shape, jnp.float32) * deviation * factor_of
    return jnp.minimum(jnp.maximum(drawn, -most), most).astype(kind)


def gaussian_with(stream_key, shape, deviation, bound, shards, heavy, kind=jnp.bfloat16):
    entries = deviation * jax.random.normal(stream_key, shape, jnp.float32)
    if shards:
        entries = entries * block_levels(stream_key, shape, shards, -0.22, 0.18)
    return jnp.clip(with_spikes(entries, jax.random.fold_in(stream_key, 3), *heavy), -bound, bound).astype(kind)


def setup_inputs(seed: int = 0) -> dict:
    arg_keys = jax.random.split(jax.random.key(seed), 15)
    moe_input = scatter_about(arg_keys[0], (TOKENS, D), 1.0, 6.0, ((0, 16),))
    out_grad = gaussian_with(arg_keys[1], (TOKENS, D), 1.0, 8.0, ((0, 16),), (0, 1, 16, 2.0))
    route_ids_keys = jax.random.split(jax.random.fold_in(arg_keys[2], 1), TOKENS // TOK_DEV)
    route_ids_turns = jax.random.permutation(jax.random.fold_in(arg_keys[2], 3), TOKENS // TOK_DEV)
    route_ids = jax.vmap(lambda own, number: deal_out(jax.random.fold_in(arg_keys[2], 2), own, number, TOK_DEV, EXPERTS, 2, CAP, 1))(route_ids_keys, route_ids_turns).reshape((TOKENS, 2))
    route_weights = jnp.clip(0.1 + 0.79999997 * jax.random.uniform(arg_keys[3], (TOKENS, 2), jnp.float32) ** block_levels(arg_keys[3], (TOKENS, 2), ((0, 16),), -0.2, 0.2), 0.1, 0.9)
    gate_w = scatter_about(arg_keys[4], (2 * EXPERTS, D, FH), D ** -0.5, 0.125, ((0, 16), (2, 2)))
    up_w = scatter_about(arg_keys[5], (2 * EXPERTS, D, FH), D ** -0.5, 0.125, ((0, 16), (2, 2)))
    down_w = scatter_about(arg_keys[6], (2 * EXPERTS, FH, D), FFE ** -0.5, 0.09375, ((0, 16), (1, 2)))
    mixer_out = scatter_about(arg_keys[7], (TOKENS, HV), 1.0, 6.0, ((0, 16), (1, 2)))
    out_weight = scatter_about(arg_keys[8], (HV, D), HV ** -0.5, 0.1875, ((0, 2),))
    queries = scatter_about(arg_keys[9], (TOKENS, HK), 0.02, 0.125, ((0, 16), (1, 2)))
    keys = scatter_about(arg_keys[10], (TOKENS, HK), 0.05, 0.3125, ((0, 16), (1, 2)))
    values = scatter_about(arg_keys[11], (TOKENS, HV), 0.25, 1.5, ((0, 16), (1, 2)))
    log_decay = draw_log_decay(jax.random.fold_in(arg_keys[14], 71), 0)
    block_states = scatter_about(arg_keys[13], (NBLK, HEADS, DK, DV), 0.3, 1.75, ((0, 16), (1, 2)), jnp.float32)
    return dict(moe_input=moe_input, out_grad=out_grad, route_ids=route_ids, route_weights=route_weights, gate_w=gate_w, up_w=up_w, down_w=down_w, mixer_out=mixer_out, out_weight=out_weight, queries=queries, keys=keys, values=values, log_decay=log_decay, block_states=block_states)


PRECISE = lax.Precision.HIGHEST
ACROSS = (((1,), (1,)), ((), ()))
DOWNWARD = (((0,), (0,)), ((), ()))


def block_back(carried, inputs):
    q_block, k_block, v_block, o_block, decay_block, state_in = inputs
    cumul = jnp.cumsum(decay_block, axis=0)
    block_total = cumul[-1]
    growth = jnp.exp(cumul)
    shrink = jnp.exp(-cumul)
    to_end = jnp.exp(block_total[None] - cumul)
    span_len = q_block.shape[0]
    causal = (jnp.arange(span_len)[:, None] >= jnp.arange(span_len)[None, :]).astype(jnp.float32)
    q_grow = q_block * growth
    k_shrink = k_block * shrink
    scores = jnp.einsum('thv,shv->hts', o_block, v_block, precision=PRECISE) * causal
    mutual = jnp.einsum('thd,shd->hts', q_grow, k_shrink, precision=PRECISE) * causal
    grad_q = growth * (jnp.einsum('thv,hdv->thd', o_block, state_in, precision=PRECISE)
                       + jnp.einsum('hts,shd->thd', scores, k_shrink, precision=PRECISE))
    grad_k = to_end * jnp.einsum('hdv,shv->shd', carried, v_block, precision=PRECISE) \
        + shrink * jnp.einsum('hts,thd->shd', scores, q_grow, precision=PRECISE)
    grad_v = jnp.einsum('shd,hdv->shv', k_block * to_end, carried, precision=PRECISE) \
        + jnp.einsum('hts,thv->shv', mutual, o_block, precision=PRECISE)
    contrib = q_block * grad_q - k_block * grad_k
    carried = jnp.exp(block_total)[:, :, None] * carried + jnp.einsum('thd,thv->hdv', q_grow, o_block, precision=PRECISE)
    return carried, (grad_q, grad_k, grad_v, contrib)


def reference(moe_input, out_grad, route_ids, route_weights, gate_w, up_w, down_w, mixer_out,
              out_weight, queries, keys, values, log_decay, block_states):
    flat_ids = route_ids.reshape(-1).astype(jnp.int32)
    one_hot = (flat_ids[:, None] == jnp.arange(EXPERTS, dtype=jnp.int32)[None, :]).astype(jnp.int32)
    counted = jnp.cumsum(one_hot.reshape(N_SP, 2 * TOK_DEV, EXPERTS), axis=1).reshape(2 * TOKENS, EXPERTS)
    earlier_count = (jnp.sum(counted * one_hot, axis=1) - 1).astype(jnp.int32)
    source = (jnp.arange(2 * TOKENS, dtype=jnp.int32) // (2 * TOK_DEV)).astype(jnp.int32)
    slot_index = (source * CAP + earlier_count).astype(jnp.int32)
    table = jnp.full((EXPERTS, SLOTS), 2 * TOKENS, jnp.int32).at[flat_ids, slot_index].set(
        jnp.arange(2 * TOKENS, dtype=jnp.int32))
    token_rows = jnp.concatenate([jnp.repeat(moe_input, 2, axis=0), jnp.zeros((1, D), jnp.bfloat16)], axis=0)
    scaled = (route_weights[:, :, None] * out_grad[:, None, :].astype(jnp.float32)).astype(jnp.bfloat16)
    grad_rows = jnp.concatenate([scaled.reshape(2 * TOKENS, D), jnp.zeros((1, D), jnp.bfloat16)], axis=0)

    def expert_back(pieces):
        gate_pair, up_pair, down_pair, picks = pieces
        tokens_in = token_rows[picks]
        grads_in = grad_rows[picks]
        half_sums = []
        gate_halves, up_halves, down_halves = [], [], []
        for half in range(2):
            partial_value = jnp.zeros((SLOTS, D), jnp.float32)
            gate_parts, up_parts, down_parts = [], [], []
            for part in range(N_TP):
                w_gate = gate_pair[half][:, part * FQ:(part + 1) * FQ]
                w_up = up_pair[half][:, part * FQ:(part + 1) * FQ]
                w_down = down_pair[half][part * FQ:(part + 1) * FQ]
                gate_pre = jnp.dot(tokens_in, w_gate, preferred_element_type=jnp.float32)
                up_pre = jnp.dot(tokens_in, w_up, preferred_element_type=jnp.float32)
                sigmoid_gate = jax.nn.sigmoid(gate_pre)
                hidden = (gate_pre * sigmoid_gate * up_pre).astype(jnp.bfloat16)
                d_hidden = lax.dot_general(grads_in, w_down, ACROSS, preferred_element_type=jnp.float32)
                d_up = (d_hidden * gate_pre * sigmoid_gate).astype(jnp.bfloat16)
                d_gate = (d_hidden * up_pre * sigmoid_gate * (1.0 + gate_pre * (1.0 - sigmoid_gate))).astype(jnp.bfloat16)
                down_parts.append(lax.dot_general(hidden, grads_in, DOWNWARD, preferred_element_type=jnp.float32).astype(jnp.bfloat16))
                gate_parts.append(lax.dot_general(tokens_in, d_gate, DOWNWARD, preferred_element_type=jnp.float32).astype(jnp.bfloat16))
                up_parts.append(lax.dot_general(tokens_in, d_up, DOWNWARD, preferred_element_type=jnp.float32).astype(jnp.bfloat16))
                piece = lax.dot_general(d_gate, w_gate, ACROSS, preferred_element_type=jnp.float32) \
                    + lax.dot_general(d_up, w_up, ACROSS, preferred_element_type=jnp.float32)
                rounded = lax.optimization_barrier(piece.astype(jnp.bfloat16))
                partial_value = partial_value + rounded.astype(jnp.float32)
            half_sums.append(partial_value.astype(jnp.bfloat16))
            gate_halves.append(jnp.concatenate(gate_parts, axis=1))
            up_halves.append(jnp.concatenate(up_parts, axis=1))
            down_halves.append(jnp.concatenate(down_parts, axis=0))
        both_halves = half_sums[0].astype(jnp.float32) + half_sums[1].astype(jnp.float32)
        return both_halves, jnp.stack(gate_halves), jnp.stack(up_halves), jnp.stack(down_halves)

    returned, gate_grad, up_grad, down_grad = lax.map(
        expert_back,
        (gate_w.reshape(EXPERTS, 2, D, FH), up_w.reshape(EXPERTS, 2, D, FH),
         down_w.reshape(EXPERTS, 2, FH, D), table))
    routed = jnp.zeros((2 * TOKENS + 1, D), jnp.float32).at[table.reshape(-1)].add(returned.reshape(-1, D))
    moe_grad = jnp.sum(routed[:-1].reshape(TOKENS, 2, D), axis=1)
    grad_mid = (out_grad.astype(jnp.float32) + moe_grad).astype(jnp.bfloat16)
    grad_out_weight = lax.dot_general(mixer_out, grad_mid, DOWNWARD, preferred_element_type=jnp.float32)
    grad_mixed = lax.dot_general(grad_mid, out_weight, ACROSS, preferred_element_type=jnp.float32).astype(jnp.bfloat16)

    def shaped(array, depth):
        return array.astype(jnp.float32).reshape(NBLK, BLK, HEADS, depth)

    inputs = (shaped(queries, DK), shaped(keys, DK), shaped(values, DV), shaped(grad_mixed, DV),
              shaped(log_decay, DK), block_states)
    zero_state = jnp.zeros((HEADS, DK, DV), jnp.float32)
    _, (grad_q, grad_k, grad_v, contrib) = lax.scan(block_back, zero_state, inputs, reverse=True)
    contrib = contrib.reshape(TOKENS, HK)
    grad_decay = jnp.flip(jnp.cumsum(jnp.flip(contrib, 0), axis=0), 0)
    return (grad_q.reshape(TOKENS, HK).astype(jnp.bfloat16),
            grad_k.reshape(TOKENS, HK).astype(jnp.bfloat16),
            grad_v.reshape(TOKENS, HV).astype(jnp.bfloat16),
            grad_decay,
            grad_out_weight,
            gate_grad.reshape(2 * EXPERTS, D, FH),
            up_grad.reshape(2 * EXPERTS, D, FH),
            down_grad.reshape(2 * EXPERTS, FH, D))
```

```python
import functools

import jax
import jax.numpy as jnp
from jax import lax
from jax.experimental import pallas as pl
from jax.experimental.pallas import tpu as pltpu
from jax.sharding import Mesh, PartitionSpec as P

MESH = pl.DeviceIdType.MESH
SP = ("ep", "pair")

DK = 64
DV = 128
BLK = 64


PRECISE = lax.Precision.HIGHEST
ACROSS = (((1,), (1,)), ((), ()))
DOWNWARD = (((0,), (0,)), ((), ()))


def sp_size():
    return lax.axis_size("ep") * lax.axis_size("pair")


def sp_index():
    return lax.axis_index("ep") * lax.axis_size("pair") + lax.axis_index("pair")


def dispatch_kernel(
    experts, width, tok_send, grad_send, tok_out, grad_out,
    local_sem, direct_send, direct_recv, pair_send, pair_recv, core_send, core_recv,
):
    e, p, t = lax.axis_index("ep"), lax.axis_index("pair"), lax.axis_index("tp")
    barrier = pltpu.get_barrier_semaphore()
    for k in range(1, experts):
        pl.semaphore_signal(
            barrier, inc=1, device_id=(lax.rem(e + k, experts), p, t), device_id_type=MESH
        )
    pl.semaphore_signal(barrier, inc=1, device_id=(e, 1 - p, t), device_id_type=MESH)
    pl.semaphore_signal(barrier, inc=1, device_id=(e, p, 1 - t), device_id_type=MESH)
    pl.semaphore_wait(barrier, experts + 1)
    columns = pl.ds(pl.multiple_of(t * width, 128), width)
    sends, outs = (tok_send, grad_send), (tok_out, grad_out)

    def direct(a, k):
        if k == 0:
            return pltpu.make_async_copy(
                sends[a].at[e], outs[a].at[p, e, :, columns], local_sem.at[a]
            )
        dest = lax.rem(e + k, experts)
        return pltpu.make_async_remote_copy(
            src_ref=sends[a].at[dest],
            dst_ref=outs[a].at[p, e, :, columns],
            send_sem=direct_send.at[a, k],
            recv_sem=direct_recv.at[a, k],
            device_id=(dest, p, t),
            device_id_type=MESH,
        )

    def passed(a, k, which, to_pair):
        source = lax.rem(e - k + experts, experts)
        place = outs[a].at[p if which == 0 else 1 - p, source, :, columns]
        return pltpu.make_async_remote_copy(
            src_ref=place,
            dst_ref=place,
            send_sem=pair_send.at[a, k] if to_pair else core_send.at[a, which, k],
            recv_sem=pair_recv.at[a, k] if to_pair else core_recv.at[a, which, k],
            device_id=(e, 1 - p, t) if to_pair else (e, p, 1 - t),
            device_id_type=MESH,
        )

    def landed_direct(a, k):
        if k == 0:
            direct(a, 0).wait()
            return
        source = lax.rem(e - k + experts, experts)
        place = outs[a].at[p, source, :, columns]
        pltpu.make_async_remote_copy(
            src_ref=place, dst_ref=place, send_sem=direct_send.at[a, k],
            recv_sem=direct_recv.at[a, k], device_id=(source, p, t), device_id_type=MESH,
        ).wait_recv()

    def landed_passed(a, k, which, from_pair):
        source = lax.rem(e - k + experts, experts)
        own = p if which == 0 else 1 - p
        if from_pair:
            place = outs[a].at[1 - p, source, :, columns]
            sems = (pair_send.at[a, k], pair_recv.at[a, k])
        else:
            other = pl.ds(pl.multiple_of((1 - t) * width, 128), width)
            place = outs[a].at[own, source, :, other]
            sems = (core_send.at[a, which, k], core_recv.at[a, which, k])
        pltpu.make_async_remote_copy(
            src_ref=place, dst_ref=place, send_sem=sems[0], recv_sem=sems[1],
            device_id=(e, 1 - p, t), device_id_type=MESH,
        ).wait_recv()

    for a in range(2):
        for k in range(experts):
            direct(a, k).start()
    steps = [(a, k) for a in range(2) for k in range(experts)]
    lag = 2
    for i in range(len(steps) + lag):
        if i < len(steps):
            a, k = steps[i]
            landed_direct(a, k)
            passed(a, k, 0, True).start()
            passed(a, k, 0, False).start()
        if i >= lag:
            a, k = steps[i - lag]
            landed_passed(a, k, 1, True)
            passed(a, k, 1, False).start()
    for a, k in steps:
        for which in range(2):
            landed_passed(a, k, which, False)
    for a, k in steps:
        if k:
            direct(a, k).wait_send()
        passed(a, k, 0, True).wait_send()
        passed(a, k, 0, False).wait_send()
        passed(a, k, 1, False).wait_send()


def dispatch_rows(token_send, grad_send):
    experts, capacity, width = token_send.shape
    out = jax.ShapeDtypeStruct((2, experts, capacity, 2 * width), token_send.dtype)
    vmem = pl.BlockSpec(memory_space=pltpu.VMEM)
    dma = pltpu.SemaphoreType.DMA
    return pl.pallas_call(
        functools.partial(dispatch_kernel, experts, width),
        out_shape=(out, out),
        in_specs=[vmem, vmem],
        out_specs=(vmem, vmem),
        scratch_shapes=[
            dma((2,)),
            dma((2, experts)),
            dma((2, experts)),
            dma((2, experts)),
            dma((2, experts)),
            dma((2, 2, experts)),
            dma((2, 2, experts)),
        ],
        compiler_params=pltpu.CompilerParams(collective_id=0, has_side_effects=True),
        name="dispatch_rows",
    )(token_send, grad_send)


def suffix_kernel(count, rows, state, out, held, result, local_sem, go_send, go_recv, back_send, back_recv):
    me = sp_index()
    t = lax.axis_index("tp")

    def place(i):
        return (lax.div(i, 2), lax.rem(i, 2), t)

    barrier = pltpu.get_barrier_semaphore()
    for k in range(1, count):
        pl.semaphore_signal(
            barrier, inc=1, device_id=place(lax.rem(me + k, count)), device_id_type=MESH
        )
    pl.semaphore_wait(barrier, count - 1)

    def go(k):
        dest = lax.rem(me + k, count)
        if k == 0:
            return pltpu.make_async_copy(state.at[me], held.at[me], local_sem.at[0])
        return pltpu.make_async_remote_copy(
            src_ref=state.at[dest], dst_ref=held.at[me], send_sem=go_send.at[k],
            recv_sem=go_recv.at[k], device_id=place(dest), device_id_type=MESH,
        )

    def back(k):
        dest = lax.rem(me + k, count)
        if k == 0:
            return pltpu.make_async_copy(result.at[me], out.at[me], local_sem.at[1])
        return pltpu.make_async_remote_copy(
            src_ref=result.at[dest], dst_ref=out.at[me], send_sem=back_send.at[k],
            recv_sem=back_recv.at[k], device_id=place(dest), device_id_type=MESH,
        )

    def landed(ref, sends, recvs, k):
        source = lax.rem(me - k + count, count)
        pltpu.make_async_remote_copy(
            src_ref=ref.at[source], dst_ref=ref.at[source], send_sem=sends.at[k],
            recv_sem=recvs.at[k], device_id=place(source), device_id_type=MESH,
        ).wait_recv()

    for k in range(count):
        go(k).start()
    go(0).wait()
    for k in range(1, count):
        landed(held, go_send, go_recv, k)
    total = jnp.zeros((rows, state.shape[-1]), jnp.float32)
    for i in range(count - 1, -1, -1):
        result[i] = total
        total = held[i, 1] * total + held[i, 0]
    for k in range(count):
        back(k).start()
    back(0).wait()
    for k in range(1, count):
        landed(out, back_send, back_recv, k)
    for k in range(1, count):
        go(k).wait_send()
        back(k).wait_send()


def suffix_states(gain, local_sum):
    count = sp_size()
    heads, dk, dv = local_sum.shape
    rows = heads * dk // count
    packed = jnp.stack(
        [
            local_sum.reshape(count, rows, dv),
            jnp.broadcast_to(gain[:, :, None], local_sum.shape).reshape(count, rows, dv),
        ],
        axis=1,
    )
    vmem = pl.BlockSpec(memory_space=pltpu.VMEM)
    dma = pltpu.SemaphoreType.DMA
    out = pl.pallas_call(
        functools.partial(suffix_kernel, count, rows),
        out_shape=jax.ShapeDtypeStruct((count, rows, dv), jnp.float32),
        in_specs=[vmem],
        out_specs=vmem,
        scratch_shapes=[
            pltpu.VMEM((count, 2, rows, dv), jnp.float32),
            pltpu.VMEM((count, rows, dv), jnp.float32),
            dma((2,)),
            dma((count,)),
            dma((count,)),
            dma((count,)),
            dma((count,)),
        ],
        compiler_params=pltpu.CompilerParams(collective_id=1, has_side_effects=True),
        name="suffix_states",
    )(packed)
    return out.reshape(local_sum.shape)


def block_back(carried, inputs):
    q_block, k_block, v_block, o_block, decay_block, state_in = inputs
    cumul = jnp.cumsum(decay_block, axis=0)
    block_total = cumul[-1]
    growth = jnp.exp(cumul)
    shrink = jnp.exp(-cumul)
    to_end = jnp.exp(block_total[None] - cumul)
    span_len = q_block.shape[0]
    causal = (jnp.arange(span_len)[:, None] >= jnp.arange(span_len)[None, :]).astype(jnp.float32)
    q_grow = q_block * growth
    k_shrink = k_block * shrink
    scores = jnp.einsum("thv,shv->hts", o_block, v_block, precision=PRECISE) * causal
    mutual = jnp.einsum("thd,shd->hts", q_grow, k_shrink, precision=PRECISE) * causal
    grad_q = growth * (
        jnp.einsum("thv,hdv->thd", o_block, state_in, precision=PRECISE)
        + jnp.einsum("hts,shd->thd", scores, k_shrink, precision=PRECISE)
    )
    grad_k = to_end * jnp.einsum(
        "hdv,shv->shd", carried, v_block, precision=PRECISE
    ) + shrink * jnp.einsum("hts,thd->shd", scores, q_grow, precision=PRECISE)
    grad_v = jnp.einsum("shd,hdv->shv", k_block * to_end, carried, precision=PRECISE) + jnp.einsum(
        "hts,thv->shv", mutual, o_block, precision=PRECISE
    )
    contrib = q_block * grad_q - k_block * grad_k
    carried = jnp.exp(block_total)[:, :, None] * carried + jnp.einsum(
        "thd,thv->hdv", q_grow, o_block, precision=PRECISE
    )
    return (carried, (grad_q, grad_k, grad_v, contrib))


def body(
    moe_input,
    out_grad,
    route_ids,
    route_weights,
    gate_w,
    up_w,
    down_w,
    mixer_out,
    out_weight,
    queries,
    keys,
    values,
    log_decay,
    block_states,
):
    sp_count = sp_size()
    experts = lax.axis_size("ep")
    pair = lax.axis_index("pair")
    tok_rows = moe_input.shape[0]
    model_width = moe_input.shape[1]
    capacity = 3 * tok_rows // experts
    flat_ids = route_ids.reshape(-1)
    one_hot = (flat_ids[:, None] == jnp.arange(experts, dtype=jnp.int32)[None, :]).astype(jnp.int32)
    earlier_count = jnp.sum(jnp.cumsum(one_hot, axis=0) * one_hot, axis=1) - 1
    slot_index = flat_ids * capacity + earlier_count
    dispatch = (
        jnp.arange(experts * capacity, dtype=jnp.int32)[:, None] == slot_index[None, :]
    ).astype(jnp.bfloat16)
    token_pick = jnp.sum(dispatch.reshape(experts * capacity, tok_rows, 2), axis=2)
    col_count = model_width // lax.axis_size("tp")
    col_start = lax.axis_index("tp") * col_count
    source_tokens = lax.dynamic_slice_in_dim(moe_input, col_start, col_count, 1)
    source_grads = lax.dynamic_slice_in_dim(out_grad, col_start, col_count, 1)
    send_width = source_tokens.shape[1]
    scaled = (route_weights[:, :, None] * source_grads[:, None, :].astype(jnp.float32)).astype(
        jnp.bfloat16
    )
    scaled = scaled.reshape(2 * tok_rows, send_width)
    token_send = jnp.dot(token_pick, source_tokens, preferred_element_type=jnp.float32).astype(
        jnp.bfloat16
    )
    grad_send = jnp.dot(dispatch, scaled, preferred_element_type=jnp.float32).astype(jnp.bfloat16)

    arrived_tokens, arrived_grads = dispatch_rows(
        token_send.reshape(experts, capacity, send_width),
        grad_send.reshape(experts, capacity, send_width),
    )
    arrived_tokens = arrived_tokens.reshape(sp_count * capacity, model_width)
    arrived_grads = arrived_grads.reshape(sp_count * capacity, model_width)
    gate_mat = gate_w[0]
    up_mat = up_w[0]
    down_mat = down_w[0]
    gate_pre = jnp.dot(arrived_tokens, gate_mat, preferred_element_type=jnp.float32)
    up_pre = jnp.dot(arrived_tokens, up_mat, preferred_element_type=jnp.float32)
    sigmoid_gate = jax.nn.sigmoid(gate_pre)
    hidden = (gate_pre * sigmoid_gate * up_pre).astype(jnp.bfloat16)
    d_hidden = lax.dot_general(arrived_grads, down_mat, ACROSS, preferred_element_type=jnp.float32)
    d_up = (d_hidden * gate_pre * sigmoid_gate).astype(jnp.bfloat16)
    d_gate = (d_hidden * up_pre * sigmoid_gate * (1.0 + gate_pre * (1.0 - sigmoid_gate))).astype(
        jnp.bfloat16
    )
    grad_down = lax.dot_general(
        hidden, arrived_grads, DOWNWARD, preferred_element_type=jnp.float32
    ).astype(jnp.bfloat16)
    grad_gate = lax.dot_general(
        arrived_tokens, d_gate, DOWNWARD, preferred_element_type=jnp.float32
    ).astype(jnp.bfloat16)
    grad_up = lax.dot_general(
        arrived_tokens, d_up, DOWNWARD, preferred_element_type=jnp.float32
    ).astype(jnp.bfloat16)
    partial_value = lax.dot_general(
        d_gate, gate_mat, ACROSS, preferred_element_type=jnp.float32
    ) + lax.dot_general(d_up, up_mat, ACROSS, preferred_element_type=jnp.float32)
    parts = partial_value.astype(jnp.bfloat16)
    own_part = lax.dynamic_slice_in_dim(parts, col_start, col_count, 1)
    other_part = lax.dynamic_slice_in_dim(parts, col_count - col_start, col_count, 1)
    core_part = lax.ppermute(other_part, "tp", [(0, 1), (1, 0)])
    half_grad = (own_part.astype(jnp.float32) + core_part.astype(jnp.float32)).astype(jnp.bfloat16)
    half_grad = half_grad.reshape(2, experts * capacity, col_count)
    kept = lax.dynamic_index_in_dim(half_grad, pair, 0, False)
    passed_on = lax.dynamic_index_in_dim(half_grad, 1 - pair, 0, False)
    pair_part = lax.ppermute(passed_on, "pair", [(0, 1), (1, 0)])
    both = (kept.astype(jnp.float32) + pair_part.astype(jnp.float32)).astype(jnp.bfloat16)
    returned = lax.all_to_all(both, "ep", split_axis=0, concat_axis=0, tiled=True)
    moe_grad = lax.dot_general(token_pick, returned, DOWNWARD, preferred_element_type=jnp.float32)
    grad_mid = (source_grads.astype(jnp.float32) + moe_grad).astype(jnp.bfloat16)
    grad_mid = lax.all_gather(grad_mid, "tp", axis=1, tiled=True)
    mixer_all = lax.all_gather(mixer_out, SP, axis=0, tiled=True)
    mid_columns = lax.all_to_all(grad_mid, SP, split_axis=1, concat_axis=0, tiled=True)
    grad_out_weight = lax.dot_general(
        mixer_all, mid_columns, DOWNWARD, preferred_element_type=jnp.float32
    )
    grad_mixed = lax.dot_general(
        grad_mid, out_weight, ACROSS, preferred_element_type=jnp.float32
    ).astype(jnp.bfloat16)
    heads_local = queries.shape[1] // DK
    blocks = tok_rows // BLK

    def shaped(array, depth):
        return array.astype(jnp.float32).reshape(blocks, BLK, heads_local, depth)

    q_blocks = shaped(queries, DK)
    k_blocks = shaped(keys, DK)
    v_blocks = shaped(values, DV)
    decay_blocks = shaped(log_decay, DK)
    inputs = (q_blocks, k_blocks, v_blocks, shaped(grad_mixed, DV), decay_blocks, block_states)
    zero_state = jnp.zeros((heads_local, DK, DV), jnp.float32)
    local_sum, (grad_q, grad_k, grad_v, contrib) = lax.scan(
        block_back, zero_state, inputs, reverse=True
    )
    cumul = jnp.cumsum(decay_blocks, axis=1)
    totals = cumul[:, -1]
    offsets = jnp.cumsum(totals, axis=0) - totals
    position = cumul + offsets[:, None]
    device_total = jnp.sum(totals, axis=0)
    fade_out = jnp.exp(device_total[None, None] - position)
    k_fade = k_blocks * fade_out
    reach_sum = jnp.einsum("nshd,nshv->hdv", k_fade, v_blocks, precision=PRECISE)
    from_right = suffix_states(jnp.exp(device_total), local_sum)
    own_terms = jnp.sum(contrib, axis=(0, 1)) - jnp.sum(reach_sum * from_right, axis=2)
    all_terms = lax.all_gather(own_terms.reshape(-1), SP)
    later = (jnp.arange(sp_count) > sp_index()).astype(jnp.float32)
    right_terms = jnp.sum(all_terms * later[:, None], axis=0)
    key_part = jnp.einsum("nshv,hdv->nshd", v_blocks, from_right, precision=PRECISE)
    grad_k = grad_k + fade_out * key_part
    grad_v = grad_v + jnp.einsum("nshd,hdv->nshv", k_fade, from_right, precision=PRECISE)
    contrib = (contrib - k_fade * key_part).reshape(tok_rows, heads_local * DK)
    grad_decay = jnp.flip(jnp.cumsum(jnp.flip(contrib, 0), axis=0), 0) + right_terms.reshape(1, -1)
    return (
        grad_q.reshape(tok_rows, heads_local * DK).astype(jnp.bfloat16),
        grad_k.reshape(tok_rows, heads_local * DK).astype(jnp.bfloat16),
        grad_v.reshape(tok_rows, heads_local * DV).astype(jnp.bfloat16),
        grad_decay,
        grad_out_weight,
        grad_gate[None],
        grad_up[None],
        grad_down[None],
    )


def solution(mesh):
    sp_count, tp_count = mesh.devices.shape
    mesh = Mesh(mesh.devices.reshape(sp_count // 2, 2, tp_count), ("ep", "pair", "tp"))
    placed = (
        P(SP, None),
        P(SP, None),
        P(SP, None),
        P(SP, None),
        P(SP, None, "tp"),
        P(SP, None, "tp"),
        P(SP, "tp", None),
        P(SP, "tp"),
        P("tp", None),
        P(SP, "tp"),
        P(SP, "tp"),
        P(SP, "tp"),
        P(SP, "tp"),
        P(SP, "tp", None, None),
    )
    return jax.shard_map(
        body,
        mesh=mesh,
        in_specs=placed,
        out_specs=(
            P(SP, "tp"),
            P(SP, "tp"),
            P(SP, "tp"),
            P(SP, "tp"),
            P("tp", SP),
            P(SP, None, "tp"),
            P(SP, None, "tp"),
            P(SP, "tp", None),
        ),
        check_vma=False,
    )
```

```python
import functools

import jax
import jax.numpy as jnp
from jax import lax
from jax.experimental import pallas as pl
from jax.experimental.pallas import tpu as pltpu
from jax.sharding import Mesh, PartitionSpec as P

MESH = pl.DeviceIdType.MESH
SP = ("ep", "pair")

DK = 64
DV = 128
BLK = 64


PRECISE = lax.Precision.HIGHEST
ACROSS = (((1,), (1,)), ((), ()))
DOWNWARD = (((0,), (0,)), ((), ()))


def sp_size():
    return lax.axis_size("ep") * lax.axis_size("pair")


def sp_index():
    return lax.axis_index("ep") * lax.axis_size("pair") + lax.axis_index("pair")


def dispatch_kernel(
    experts, width, tok_send, grad_send, tok_out, grad_out,
    local_sem, direct_send, direct_recv, pair_send, pair_recv, core_send, core_recv,
):
    e, p, t = lax.axis_index("ep"), lax.axis_index("pair"), lax.axis_index("tp")
    barrier = pltpu.get_barrier_semaphore()
    for k in range(1, experts):
        pl.semaphore_signal(
            barrier, inc=1, device_id=(lax.rem(e + k, experts), p, t), device_id_type=MESH
        )
    pl.semaphore_signal(barrier, inc=1, device_id=(e, 1 - p, t), device_id_type=MESH)
    pl.semaphore_signal(barrier, inc=1, device_id=(e, p, 1 - t), device_id_type=MESH)
    pl.semaphore_wait(barrier, experts + 1)
    columns = pl.ds(pl.multiple_of(t * width, 128), width)
    sends, outs = (tok_send, grad_send), (tok_out, grad_out)

    def direct(a, k):
        if k == 0:
            return pltpu.make_async_copy(
                sends[a].at[e], outs[a].at[p, e, :, columns], local_sem.at[a]
            )
        dest = lax.rem(e + k, experts)
        return pltpu.make_async_remote_copy(
            src_ref=sends[a].at[dest],
            dst_ref=outs[a].at[p, e, :, columns],
            send_sem=direct_send.at[a, k],
            recv_sem=direct_recv.at[a, k],
            device_id=(dest, p, t),
            device_id_type=MESH,
        )

    def passed(a, k, which, to_pair):
        source = lax.rem(e - k + experts, experts)
        place = outs[a].at[p if which == 0 else 1 - p, source, :, columns]
        return pltpu.make_async_remote_copy(
            src_ref=place,
            dst_ref=place,
            send_sem=pair_send.at[a, k] if to_pair else core_send.at[a, which, k],
            recv_sem=pair_recv.at[a, k] if to_pair else core_recv.at[a, which, k],
            device_id=(e, 1 - p, t) if to_pair else (e, p, 1 - t),
            device_id_type=MESH,
        )

    def landed_direct(a, k):
        if k == 0:
            direct(a, 0).wait()
            return
        source = lax.rem(e - k + experts, experts)
        place = outs[a].at[p, source, :, columns]
        pltpu.make_async_remote_copy(
            src_ref=place, dst_ref=place, send_sem=direct_send.at[a, k],
            recv_sem=direct_recv.at[a, k], device_id=(source, p, t), device_id_type=MESH,
        ).wait_recv()

    def landed_passed(a, k, which, from_pair):
        source = lax.rem(e - k + experts, experts)
        own = p if which == 0 else 1 - p
        if from_pair:
            place = outs[a].at[1 - p, source, :, columns]
            sems = (pair_send.at[a, k], pair_recv.at[a, k])
        else:
            other = pl.ds(pl.multiple_of((1 - t) * width, 128), width)
            place = outs[a].at[own, source, :, other]
            sems = (core_send.at[a, which, k], core_recv.at[a, which, k])
        pltpu.make_async_remote_copy(
            src_ref=place, dst_ref=place, send_sem=sems[0], recv_sem=sems[1],
            device_id=(e, 1 - p, t), device_id_type=MESH,
        ).wait_recv()

    for a in range(2):
        for k in range(experts):
            direct(a, k).start()
    steps = [(a, k) for a in range(2) for k in range(experts)]
    lag = 2
    for i in range(len(steps) + lag):
        if i < len(steps):
            a, k = steps[i]
            landed_direct(a, k)
            passed(a, k, 0, True).start()
            passed(a, k, 0, False).start()
        if i >= lag:
            a, k = steps[i - lag]
            landed_passed(a, k, 1, True)
            passed(a, k, 1, False).start()
    for a, k in steps:
        for which in range(2):
            landed_passed(a, k, which, False)
    for a, k in steps:
        if k:
            direct(a, k).wait_send()
        passed(a, k, 0, True).wait_send()
        passed(a, k, 0, False).wait_send()
        passed(a, k, 1, False).wait_send()


def dispatch_rows(token_send, grad_send):
    experts, capacity, width = token_send.shape
    out = jax.ShapeDtypeStruct((2, experts, capacity, 2 * width), token_send.dtype)
    vmem = pl.BlockSpec(memory_space=pltpu.VMEM)
    dma = pltpu.SemaphoreType.DMA
    return pl.pallas_call(
        functools.partial(dispatch_kernel, experts, width),
        out_shape=(out, out),
        in_specs=[vmem, vmem],
        out_specs=(vmem, vmem),
        scratch_shapes=[
            dma((2,)),
            dma((2, experts)),
            dma((2, experts)),
            dma((2, experts)),
            dma((2, experts)),
            dma((2, 2, experts)),
            dma((2, 2, experts)),
        ],
        compiler_params=pltpu.CompilerParams(collective_id=0, has_side_effects=True),
        name="dispatch_rows",
    )(token_send, grad_send)


def suffix_kernel(
    count, rows, state, reach, terms, out, right, held, result, gathered,
    local_sem, go_send, go_recv, back_send, back_recv, term_send, term_recv,
):
    me = sp_index()
    t = lax.axis_index("tp")

    def place(i):
        return (lax.div(i, 2), lax.rem(i, 2), t)

    barrier = pltpu.get_barrier_semaphore()
    for k in range(1, count):
        pl.semaphore_signal(
            barrier, inc=1, device_id=place(lax.rem(me + k, count)), device_id_type=MESH
        )
    pl.semaphore_wait(barrier, count - 1)

    def go(k):
        dest = lax.rem(me + k, count)
        if k == 0:
            return pltpu.make_async_copy(state.at[me], held.at[me], local_sem.at[0])
        return pltpu.make_async_remote_copy(
            src_ref=state.at[dest], dst_ref=held.at[me], send_sem=go_send.at[k],
            recv_sem=go_recv.at[k], device_id=place(dest), device_id_type=MESH,
        )

    def back(k):
        dest = lax.rem(me + k, count)
        if k == 0:
            return pltpu.make_async_copy(result.at[me], out.at[me], local_sem.at[1])
        return pltpu.make_async_remote_copy(
            src_ref=result.at[dest], dst_ref=out.at[me], send_sem=back_send.at[k],
            recv_sem=back_recv.at[k], device_id=place(dest), device_id_type=MESH,
        )

    def landed(ref, sends, recvs, k):
        source = lax.rem(me - k + count, count)
        pltpu.make_async_remote_copy(
            src_ref=ref.at[source], dst_ref=ref.at[source], send_sem=sends.at[k],
            recv_sem=recvs.at[k], device_id=place(source), device_id_type=MESH,
        ).wait_recv()

    for k in range(count):
        go(k).start()
    go(0).wait()
    for k in range(1, count):
        landed(held, go_send, go_recv, k)
    total = jnp.zeros((rows, state.shape[-1]), jnp.float32)
    for i in range(count - 1, -1, -1):
        result[i] = total
        total = held[i, 1] * total + held[i, 0]
    for k in range(count):
        back(k).start()
    back(0).wait()
    for k in range(1, count):
        landed(out, back_send, back_recv, k)
    lanes = lax.broadcasted_iota(jnp.int32, (rows, state.shape[-1]), 1)
    places = lax.broadcasted_iota(jnp.int32, (rows, state.shape[-1]), 0)
    groups = [jnp.zeros((1, 128), jnp.float32) for _ in range(terms.shape[0])]
    for c in range(count):
        dots = jnp.sum(reach[c] * out[c], axis=1, keepdims=True)
        picked = jnp.where(lanes == places + (c * rows) % 128, dots, 0.0)
        groups[c * rows // 128] += jnp.sum(picked, axis=0, keepdims=True)
    gathered[me] = terms[...] - jnp.concatenate(groups, axis=0)

    def tell(k):
        return pltpu.make_async_remote_copy(
            src_ref=gathered.at[me], dst_ref=gathered.at[me], send_sem=term_send.at[k],
            recv_sem=term_recv.at[k], device_id=place(lax.rem(me + k, count)), device_id_type=MESH,
        )

    for k in range(1, count):
        go(k).wait_send()
        back(k).wait_send()
    for k in range(1, count):
        tell(k).start()
    for k in range(1, count):
        landed(gathered, term_send, term_recv, k)
    summed = jnp.zeros(terms.shape, jnp.float32)
    for i in range(count):
        summed += jnp.where(i > me, gathered[i], 0.0)
    right[...] = summed
    for k in range(1, count):
        tell(k).wait_send()


def suffix_states(gain, local_sum, reach_sum, terms):
    count = sp_size()
    heads, dk, dv = local_sum.shape
    rows = heads * dk // count
    packed = jnp.stack(
        [
            local_sum.reshape(count, rows, dv),
            jnp.broadcast_to(gain[:, :, None], local_sum.shape).reshape(count, rows, dv),
        ],
        axis=1,
    )
    vmem = pl.BlockSpec(memory_space=pltpu.VMEM)
    dma = pltpu.SemaphoreType.DMA
    terms = terms.reshape(heads * dk // 128, 128)
    out, right = pl.pallas_call(
        functools.partial(suffix_kernel, count, rows),
        out_shape=(
            jax.ShapeDtypeStruct((count, rows, dv), jnp.float32),
            jax.ShapeDtypeStruct(terms.shape, jnp.float32),
        ),
        in_specs=[vmem] * 3,
        out_specs=(vmem, vmem),
        scratch_shapes=[
            pltpu.VMEM((count, 2, rows, dv), jnp.float32),
            pltpu.VMEM((count, rows, dv), jnp.float32),
            pltpu.VMEM((count,) + terms.shape, jnp.float32),
            dma((2,)),
            dma((count,)),
            dma((count,)),
            dma((count,)),
            dma((count,)),
            dma((count,)),
            dma((count,)),
        ],
        compiler_params=pltpu.CompilerParams(collective_id=1, has_side_effects=True),
        name="suffix_states",
    )(packed, reach_sum.reshape(count, rows, dv), terms)
    return out.reshape(local_sum.shape), right.reshape(1, -1)


def return_kernel(
    experts, width, steps, parts, tokens, grads, hidden, d_gate, d_up,
    returned, gate_out, up_out, down_out,
    core_held, pair_stage, pair_held, send_stage, gate_stage, up_stage, down_stage,
    out_sem, local_sem, core_send, core_recv, pair_send, pair_recv, back_send, back_recv,
):
    e, p, t = lax.axis_index("ep"), lax.axis_index("pair"), lax.axis_index("tp")
    barrier = pltpu.get_barrier_semaphore()
    for k in range(1, experts):
        pl.semaphore_signal(
            barrier, inc=1, device_id=(lax.rem(e + k, experts), p, t), device_id_type=MESH
        )
    pl.semaphore_signal(barrier, inc=1, device_id=(e, 1 - p, t), device_id_type=MESH)
    pl.semaphore_signal(barrier, inc=1, device_id=(e, p, 1 - t), device_id_type=MESH)
    pl.semaphore_wait(barrier, experts + 1)
    own_columns = pl.ds(pl.multiple_of(t * width, 128), width)
    core_columns = pl.ds(pl.multiple_of((1 - t) * width, 128), width)

    def owner(k):
        return lax.rem(e + 1 + k, experts)

    def core_copy(which, k):
        side = 1 - p if which == 0 else p
        return pltpu.make_async_remote_copy(
            src_ref=parts.at[side, owner(k), :, core_columns],
            dst_ref=core_held.at[which, k],
            send_sem=core_send.at[which, k],
            recv_sem=core_recv.at[which, k],
            device_id=(e, p, 1 - t),
            device_id_type=MESH,
        )

    def pair_copy(k):
        return pltpu.make_async_remote_copy(
            src_ref=pair_stage.at[k], dst_ref=pair_held.at[k], send_sem=pair_send.at[k],
            recv_sem=pair_recv.at[k], device_id=(e, 1 - p, t), device_id_type=MESH,
        )

    def back_copy(k):
        return pltpu.make_async_remote_copy(
            src_ref=send_stage.at[k], dst_ref=returned.at[e], send_sem=back_send.at[k],
            recv_sem=back_recv.at[k], device_id=(owner(k), p, t), device_id_type=MESH,
        )

    def half_of(which, k):
        side = 1 - p if which == 0 else p
        mine = parts[side, owner(k), :, own_columns].astype(jnp.float32)
        return (mine + core_held[which, k].astype(jnp.float32)).astype(jnp.bfloat16)

    for which in range(2):
        for k in range(experts):
            core_copy(which, k).start()
    for k in range(experts):
        core_copy(0, k).wait_recv()
        pair_stage[k] = half_of(0, k)
        if k:
            pair_copy(k - 1).start()
    pair_copy(experts - 1).start()
    for k in range(experts):
        core_copy(1, k).wait_recv()

    def down_step(i, carry):
        cut = pl.ds(pl.multiple_of(i * 128, 128), 128)
        down_stage[cut, :] = lax.dot_general(
            hidden[:, cut], grads[...], DOWNWARD, preferred_element_type=jnp.float32
        ).astype(jnp.bfloat16)
        pltpu.make_async_copy(down_stage.at[cut], down_out.at[cut], out_sem.at[0]).start()
        return carry

    lax.fori_loop(0, hidden.shape[1] // 128, down_step, 0)
    span = tokens.shape[1] // steps
    each = experts // steps

    def weight_step(i, carry):
        cut = pl.ds(pl.multiple_of(i * span, span), span)
        gate_stage[cut, :] = lax.dot_general(
            tokens[:, cut], d_gate[...], DOWNWARD, preferred_element_type=jnp.float32
        ).astype(jnp.bfloat16)
        for j in range(each):
            k = i * each + j
            pair_copy(k).wait_recv()
            total = half_of(1, k).astype(jnp.float32) + pair_held[k].astype(jnp.float32)
            send_stage[k] = total.astype(jnp.bfloat16)
        up_stage[cut, :] = lax.dot_general(
            tokens[:, cut], d_up[...], DOWNWARD, preferred_element_type=jnp.float32
        ).astype(jnp.bfloat16)
        for j in range(each):
            k = i * each + j

            @pl.when(k < experts - 1)
            def _():
                back_copy(k).start()

        pltpu.make_async_copy(gate_stage.at[cut], gate_out.at[cut], out_sem.at[1]).start()
        pltpu.make_async_copy(up_stage.at[cut], up_out.at[cut], out_sem.at[2]).start()
        return carry

    lax.fori_loop(0, steps, weight_step, 0)
    own = pltpu.make_async_copy(send_stage.at[experts - 1], returned.at[e], local_sem)
    own.start()
    own.wait()
    for k in range(experts - 1):
        source = lax.rem(e - 1 - k + experts, experts)
        pltpu.make_async_remote_copy(
            src_ref=returned.at[source], dst_ref=returned.at[source], send_sem=back_send.at[k],
            recv_sem=back_recv.at[k], device_id=(source, p, t), device_id_type=MESH,
        ).wait_recv()
    for k in range(experts):
        core_copy(0, k).wait_send()
        core_copy(1, k).wait_send()
        pair_copy(k).wait_send()
        if k < experts - 1:
            back_copy(k).wait_send()
    pltpu.make_async_copy(down_stage, down_out, out_sem.at[0]).wait()
    pltpu.make_async_copy(gate_stage, gate_out, out_sem.at[1]).wait()
    pltpu.make_async_copy(up_stage, up_out, out_sem.at[2]).wait()


def return_rows(parts, tokens, grads, hidden, d_gate, d_up):
    _, experts, capacity, model_width = parts.shape
    width = model_width // 2
    units = hidden.shape[1]
    half = (experts, capacity, width)
    vmem = pl.BlockSpec(memory_space=pltpu.VMEM)
    hbm = pl.BlockSpec(memory_space=pl.ANY)
    dma = pltpu.SemaphoreType.DMA
    wide, tall = (model_width, units), (units, model_width)
    kind = jnp.bfloat16
    shape = jax.ShapeDtypeStruct
    return pl.pallas_call(
        functools.partial(return_kernel, experts, width, min(8, experts)),
        out_shape=(shape(half, kind), shape(wide, kind), shape(wide, kind), shape(tall, kind)),
        in_specs=[vmem] * 6,
        out_specs=(vmem, hbm, hbm, hbm),
        scratch_shapes=[
            pltpu.VMEM((2,) + half, kind),
            pltpu.VMEM(half, kind),
            pltpu.VMEM(half, kind),
            pltpu.VMEM(half, kind),
            pltpu.VMEM(wide, kind),
            pltpu.VMEM(wide, kind),
            pltpu.VMEM(tall, kind),
            dma((3,)),
            dma,
            dma((2, experts)),
            dma((2, experts)),
            dma((experts,)),
            dma((experts,)),
            dma((experts,)),
            dma((experts,)),
        ],
        compiler_params=pltpu.CompilerParams(
            collective_id=2, has_side_effects=True, vmem_limit_bytes=60 * 1024 * 1024
        ),
        name="return_rows",
    )(parts, tokens, grads, hidden, d_gate, d_up)


def block_back(carried, inputs):
    q_block, k_block, v_block, o_block, decay_block, state_in = inputs
    cumul = jnp.cumsum(decay_block, axis=0)
    block_total = cumul[-1]
    growth = jnp.exp(cumul)
    shrink = jnp.exp(-cumul)
    to_end = jnp.exp(block_total[None] - cumul)
    span_len = q_block.shape[0]
    causal = (jnp.arange(span_len)[:, None] >= jnp.arange(span_len)[None, :]).astype(jnp.float32)
    q_grow = q_block * growth
    k_shrink = k_block * shrink
    scores = jnp.einsum("thv,shv->hts", o_block, v_block, precision=PRECISE) * causal
    mutual = jnp.einsum("thd,shd->hts", q_grow, k_shrink, precision=PRECISE) * causal
    grad_q = growth * (
        jnp.einsum("thv,hdv->thd", o_block, state_in, precision=PRECISE)
        + jnp.einsum("hts,shd->thd", scores, k_shrink, precision=PRECISE)
    )
    grad_k = to_end * jnp.einsum(
        "hdv,shv->shd", carried, v_block, precision=PRECISE
    ) + shrink * jnp.einsum("hts,thd->shd", scores, q_grow, precision=PRECISE)
    grad_v = jnp.einsum("shd,hdv->shv", k_block * to_end, carried, precision=PRECISE) + jnp.einsum(
        "hts,thv->shv", mutual, o_block, precision=PRECISE
    )
    contrib = q_block * grad_q - k_block * grad_k
    carried = jnp.exp(block_total)[:, :, None] * carried + jnp.einsum(
        "thd,thv->hdv", q_grow, o_block, precision=PRECISE
    )
    return (carried, (grad_q, grad_k, grad_v, contrib))


def body(
    moe_input,
    out_grad,
    route_ids,
    route_weights,
    gate_w,
    up_w,
    down_w,
    mixer_out,
    out_weight,
    queries,
    keys,
    values,
    log_decay,
    block_states,
):
    sp_count = sp_size()
    experts = lax.axis_size("ep")
    tok_rows = moe_input.shape[0]
    model_width = moe_input.shape[1]
    capacity = 3 * tok_rows // experts
    flat_ids = route_ids.reshape(-1)
    one_hot = (flat_ids[:, None] == jnp.arange(experts, dtype=jnp.int32)[None, :]).astype(jnp.int32)
    earlier_count = jnp.sum(jnp.cumsum(one_hot, axis=0) * one_hot, axis=1) - 1
    slot_index = flat_ids * capacity + earlier_count
    dispatch = (
        jnp.arange(experts * capacity, dtype=jnp.int32)[:, None] == slot_index[None, :]
    ).astype(jnp.bfloat16)
    token_pick = jnp.sum(dispatch.reshape(experts * capacity, tok_rows, 2), axis=2)
    col_count = model_width // lax.axis_size("tp")
    col_start = lax.axis_index("tp") * col_count
    source_tokens = lax.dynamic_slice_in_dim(moe_input, col_start, col_count, 1)
    source_grads = lax.dynamic_slice_in_dim(out_grad, col_start, col_count, 1)
    send_width = source_tokens.shape[1]
    scaled = (route_weights[:, :, None] * source_grads[:, None, :].astype(jnp.float32)).astype(
        jnp.bfloat16
    )
    scaled = scaled.reshape(2 * tok_rows, send_width)
    token_send = jnp.dot(token_pick, source_tokens, preferred_element_type=jnp.float32).astype(
        jnp.bfloat16
    )
    grad_send = jnp.dot(dispatch, scaled, preferred_element_type=jnp.float32).astype(jnp.bfloat16)

    arrived_tokens, arrived_grads = dispatch_rows(
        token_send.reshape(experts, capacity, send_width),
        grad_send.reshape(experts, capacity, send_width),
    )
    arrived_tokens = arrived_tokens.reshape(sp_count * capacity, model_width)
    arrived_grads = arrived_grads.reshape(sp_count * capacity, model_width)
    gate_mat = gate_w[0]
    up_mat = up_w[0]
    down_mat = down_w[0]
    gate_pre = jnp.dot(arrived_tokens, gate_mat, preferred_element_type=jnp.float32)
    up_pre = jnp.dot(arrived_tokens, up_mat, preferred_element_type=jnp.float32)
    sigmoid_gate = jax.nn.sigmoid(gate_pre)
    hidden = (gate_pre * sigmoid_gate * up_pre).astype(jnp.bfloat16)
    d_hidden = lax.dot_general(arrived_grads, down_mat, ACROSS, preferred_element_type=jnp.float32)
    d_up = (d_hidden * gate_pre * sigmoid_gate).astype(jnp.bfloat16)
    d_gate = (d_hidden * up_pre * sigmoid_gate * (1.0 + gate_pre * (1.0 - sigmoid_gate))).astype(
        jnp.bfloat16
    )
    partial_value = lax.dot_general(
        d_gate, gate_mat, ACROSS, preferred_element_type=jnp.float32
    ) + lax.dot_general(d_up, up_mat, ACROSS, preferred_element_type=jnp.float32)
    parts = partial_value.astype(jnp.bfloat16)
    returned, grad_gate, grad_up, grad_down = return_rows(
        parts.reshape(2, experts, capacity, model_width),
        arrived_tokens,
        arrived_grads,
        hidden,
        d_gate,
        d_up,
    )
    returned = returned.reshape(experts * capacity, col_count)
    moe_grad = lax.dot_general(token_pick, returned, DOWNWARD, preferred_element_type=jnp.float32)
    grad_mid = (source_grads.astype(jnp.float32) + moe_grad).astype(jnp.bfloat16)
    grad_mid = lax.all_gather(grad_mid, "tp", axis=1, tiled=True)
    mixer_all = lax.all_gather(mixer_out, SP, axis=0, tiled=True)
    mid_columns = lax.all_to_all(grad_mid, SP, split_axis=1, concat_axis=0, tiled=True)
    grad_out_weight = lax.dot_general(
        mixer_all, mid_columns, DOWNWARD, preferred_element_type=jnp.float32
    )
    grad_mixed = lax.dot_general(
        grad_mid, out_weight, ACROSS, preferred_element_type=jnp.float32
    ).astype(jnp.bfloat16)
    heads_local = queries.shape[1] // DK
    blocks = tok_rows // BLK

    def shaped(array, depth):
        return array.astype(jnp.float32).reshape(blocks, BLK, heads_local, depth)

    q_blocks = shaped(queries, DK)
    k_blocks = shaped(keys, DK)
    v_blocks = shaped(values, DV)
    decay_blocks = shaped(log_decay, DK)
    inputs = (q_blocks, k_blocks, v_blocks, shaped(grad_mixed, DV), decay_blocks, block_states)
    zero_state = jnp.zeros((heads_local, DK, DV), jnp.float32)
    local_sum, (grad_q, grad_k, grad_v, contrib) = lax.scan(
        block_back, zero_state, inputs, reverse=True
    )
    cumul = jnp.cumsum(decay_blocks, axis=1)
    totals = cumul[:, -1]
    offsets = jnp.cumsum(totals, axis=0) - totals
    position = cumul + offsets[:, None]
    device_total = jnp.sum(totals, axis=0)
    fade_out = jnp.exp(device_total[None, None] - position)
    k_fade = k_blocks * fade_out
    reach_sum = jnp.einsum("nshd,nshv->hdv", k_fade, v_blocks, precision=PRECISE)
    from_right, right_terms = suffix_states(
        jnp.exp(device_total), local_sum, reach_sum, jnp.sum(contrib, axis=(0, 1))
    )
    key_part = jnp.einsum("nshv,hdv->nshd", v_blocks, from_right, precision=PRECISE)
    grad_k = grad_k + fade_out * key_part
    grad_v = grad_v + jnp.einsum("nshd,hdv->nshv", k_fade, from_right, precision=PRECISE)
    contrib = (contrib - k_fade * key_part).reshape(tok_rows, heads_local * DK)
    grad_decay = jnp.flip(jnp.cumsum(jnp.flip(contrib, 0), axis=0), 0) + right_terms
    return (
        grad_q.reshape(tok_rows, heads_local * DK).astype(jnp.bfloat16),
        grad_k.reshape(tok_rows, heads_local * DK).astype(jnp.bfloat16),
        grad_v.reshape(tok_rows, heads_local * DV).astype(jnp.bfloat16),
        grad_decay,
        grad_out_weight,
        grad_gate[None],
        grad_up[None],
        grad_down[None],
    )


def solution(mesh):
    sp_count, tp_count = mesh.devices.shape
    mesh = Mesh(mesh.devices.reshape(sp_count // 2, 2, tp_count), ("ep", "pair", "tp"))
    placed = (
        P(SP, None),
        P(SP, None),
        P(SP, None),
        P(SP, None),
        P(SP, None, "tp"),
        P(SP, None, "tp"),
        P(SP, "tp", None),
        P(SP, "tp"),
        P("tp", None),
        P(SP, "tp"),
        P(SP, "tp"),
        P(SP, "tp"),
        P(SP, "tp"),
        P(SP, "tp", None, None),
    )
    return jax.shard_map(
        body,
        mesh=mesh,
        in_specs=placed,
        out_specs=(
            P(SP, "tp"),
            P(SP, "tp"),
            P(SP, "tp"),
            P(SP, "tp"),
            P("tp", SP),
            P(SP, None, "tp"),
            P(SP, None, "tp"),
            P(SP, "tp", None),
        ),
        check_vma=False,
    )
```

```python
import functools

import jax
import jax.numpy as jnp
from jax import lax
from jax.experimental import pallas as pl
from jax.experimental.pallas import tpu as pltpu
from jax.sharding import Mesh, PartitionSpec as P

MESH = pl.DeviceIdType.MESH
SP = ("ep", "pair")

DK = 64
DV = 128
BLK = 64


PRECISE = lax.Precision.HIGHEST
ACROSS = (((1,), (1,)), ((), ()))
DOWNWARD = (((0,), (0,)), ((), ()))


def sp_size():
    return lax.axis_size("ep") * lax.axis_size("pair")


def sp_index():
    return lax.axis_index("ep") * lax.axis_size("pair") + lax.axis_index("pair")


def dispatch_kernel(
    experts, width, tok_send, grad_send, tok_out, grad_out,
    local_sem, direct_send, direct_recv, pair_send, pair_recv, core_send, core_recv,
):
    e, p, t = lax.axis_index("ep"), lax.axis_index("pair"), lax.axis_index("tp")
    barrier = pltpu.get_barrier_semaphore()
    for k in range(1, experts):
        pl.semaphore_signal(
            barrier, inc=1, device_id=(lax.rem(e + k, experts), p, t), device_id_type=MESH
        )
    pl.semaphore_signal(barrier, inc=1, device_id=(e, 1 - p, t), device_id_type=MESH)
    pl.semaphore_signal(barrier, inc=1, device_id=(e, p, 1 - t), device_id_type=MESH)
    pl.semaphore_wait(barrier, experts + 1)
    columns = pl.ds(pl.multiple_of(t * width, 128), width)
    sends, outs = (tok_send, grad_send), (tok_out, grad_out)

    def direct(a, k):
        if k == 0:
            return pltpu.make_async_copy(
                sends[a].at[e], outs[a].at[p, e, :, columns], local_sem.at[a]
            )
        dest = lax.rem(e + k, experts)
        return pltpu.make_async_remote_copy(
            src_ref=sends[a].at[dest],
            dst_ref=outs[a].at[p, e, :, columns],
            send_sem=direct_send.at[a, k],
            recv_sem=direct_recv.at[a, k],
            device_id=(dest, p, t),
            device_id_type=MESH,
        )

    def passed(a, k, which, to_pair):
        source = lax.rem(e - k + experts, experts)
        place = outs[a].at[p if which == 0 else 1 - p, source, :, columns]
        return pltpu.make_async_remote_copy(
            src_ref=place,
            dst_ref=place,
            send_sem=pair_send.at[a, k] if to_pair else core_send.at[a, which, k],
            recv_sem=pair_recv.at[a, k] if to_pair else core_recv.at[a, which, k],
            device_id=(e, 1 - p, t) if to_pair else (e, p, 1 - t),
            device_id_type=MESH,
        )

    def landed_direct(a, k):
        if k == 0:
            direct(a, 0).wait()
            return
        source = lax.rem(e - k + experts, experts)
        place = outs[a].at[p, source, :, columns]
        pltpu.make_async_remote_copy(
            src_ref=place, dst_ref=place, send_sem=direct_send.at[a, k],
            recv_sem=direct_recv.at[a, k], device_id=(source, p, t), device_id_type=MESH,
        ).wait_recv()

    def landed_passed(a, k, which, from_pair):
        source = lax.rem(e - k + experts, experts)
        own = p if which == 0 else 1 - p
        if from_pair:
            place = outs[a].at[1 - p, source, :, columns]
            sems = (pair_send.at[a, k], pair_recv.at[a, k])
        else:
            other = pl.ds(pl.multiple_of((1 - t) * width, 128), width)
            place = outs[a].at[own, source, :, other]
            sems = (core_send.at[a, which, k], core_recv.at[a, which, k])
        pltpu.make_async_remote_copy(
            src_ref=place, dst_ref=place, send_sem=sems[0], recv_sem=sems[1],
            device_id=(e, 1 - p, t), device_id_type=MESH,
        ).wait_recv()

    for a in range(2):
        for k in range(experts):
            direct(a, k).start()
    steps = [(a, k) for a in range(2) for k in range(experts)]
    lag = 2
    for i in range(len(steps) + lag):
        if i < len(steps):
            a, k = steps[i]
            landed_direct(a, k)
            passed(a, k, 0, True).start()
            passed(a, k, 0, False).start()
        if i >= lag:
            a, k = steps[i - lag]
            landed_passed(a, k, 1, True)
            passed(a, k, 1, False).start()
    for a, k in steps:
        for which in range(2):
            landed_passed(a, k, which, False)
    for a, k in steps:
        if k:
            direct(a, k).wait_send()
        passed(a, k, 0, True).wait_send()
        passed(a, k, 0, False).wait_send()
        passed(a, k, 1, False).wait_send()


def dispatch_rows(token_send, grad_send):
    experts, capacity, width = token_send.shape
    out = jax.ShapeDtypeStruct((2, experts, capacity, 2 * width), token_send.dtype)
    vmem = pl.BlockSpec(memory_space=pltpu.VMEM)
    dma = pltpu.SemaphoreType.DMA
    return pl.pallas_call(
        functools.partial(dispatch_kernel, experts, width),
        out_shape=(out, out),
        in_specs=[vmem, vmem],
        out_specs=(vmem, vmem),
        scratch_shapes=[
            dma((2,)),
            dma((2, experts)),
            dma((2, experts)),
            dma((2, experts)),
            dma((2, experts)),
            dma((2, 2, experts)),
            dma((2, 2, experts)),
        ],
        compiler_params=pltpu.CompilerParams(collective_id=0, has_side_effects=True),
        name="dispatch_rows",
    )(token_send, grad_send)


def suffix_kernel(
    count, rows, state, reach, terms, out, right, held, result, gathered,
    local_sem, go_send, go_recv, back_send, back_recv, term_send, term_recv,
):
    me = sp_index()
    t = lax.axis_index("tp")

    def place(i):
        return (lax.div(i, 2), lax.rem(i, 2), t)

    barrier = pltpu.get_barrier_semaphore()
    for k in range(1, count):
        pl.semaphore_signal(
            barrier, inc=1, device_id=place(lax.rem(me + k, count)), device_id_type=MESH
        )
    pl.semaphore_wait(barrier, count - 1)

    def go(k):
        dest = lax.rem(me + k, count)
        if k == 0:
            return pltpu.make_async_copy(state.at[me], held.at[me], local_sem.at[0])
        return pltpu.make_async_remote_copy(
            src_ref=state.at[dest], dst_ref=held.at[me], send_sem=go_send.at[k],
            recv_sem=go_recv.at[k], device_id=place(dest), device_id_type=MESH,
        )

    def back(k):
        dest = lax.rem(me + k, count)
        if k == 0:
            return pltpu.make_async_copy(result.at[me], out.at[me], local_sem.at[1])
        return pltpu.make_async_remote_copy(
            src_ref=result.at[dest], dst_ref=out.at[me], send_sem=back_send.at[k],
            recv_sem=back_recv.at[k], device_id=place(dest), device_id_type=MESH,
        )

    def landed(ref, sends, recvs, k):
        source = lax.rem(me - k + count, count)
        pltpu.make_async_remote_copy(
            src_ref=ref.at[source], dst_ref=ref.at[source], send_sem=sends.at[k],
            recv_sem=recvs.at[k], device_id=place(source), device_id_type=MESH,
        ).wait_recv()

    for k in range(count):
        go(k).start()
    go(0).wait()
    for k in range(1, count):
        landed(held, go_send, go_recv, k)
    total = jnp.zeros((rows, state.shape[-1]), jnp.float32)
    for i in range(count - 1, -1, -1):
        result[i] = total
        total = held[i, 1] * total + held[i, 0]
    for k in range(count):
        back(k).start()
    back(0).wait()
    for k in range(1, count):
        landed(out, back_send, back_recv, k)
    lanes = lax.broadcasted_iota(jnp.int32, (rows, state.shape[-1]), 1)
    places = lax.broadcasted_iota(jnp.int32, (rows, state.shape[-1]), 0)
    groups = [jnp.zeros((1, 128), jnp.float32) for _ in range(terms.shape[0])]
    for c in range(count):
        dots = jnp.sum(reach[c] * out[c], axis=1, keepdims=True)
        picked = jnp.where(lanes == places + (c * rows) % 128, dots, 0.0)
        groups[c * rows // 128] += jnp.sum(picked, axis=0, keepdims=True)
    gathered[me] = terms[...] - jnp.concatenate(groups, axis=0)

    def tell(k):
        return pltpu.make_async_remote_copy(
            src_ref=gathered.at[me], dst_ref=gathered.at[me], send_sem=term_send.at[k],
            recv_sem=term_recv.at[k], device_id=place(lax.rem(me + k, count)), device_id_type=MESH,
        )

    for k in range(1, count):
        go(k).wait_send()
        back(k).wait_send()
    for k in range(1, count):
        tell(k).start()
    for k in range(1, count):
        landed(gathered, term_send, term_recv, k)
    summed = jnp.zeros(terms.shape, jnp.float32)
    for i in range(count):
        summed += jnp.where(i > me, gathered[i], 0.0)
    right[...] = summed
    for k in range(1, count):
        tell(k).wait_send()


def suffix_states(gain, local_sum, reach_sum, terms):
    count = sp_size()
    heads, dk, dv = local_sum.shape
    rows = heads * dk // count
    packed = jnp.stack(
        [
            local_sum.reshape(count, rows, dv),
            jnp.broadcast_to(gain[:, :, None], local_sum.shape).reshape(count, rows, dv),
        ],
        axis=1,
    )
    vmem = pl.BlockSpec(memory_space=pltpu.VMEM)
    dma = pltpu.SemaphoreType.DMA
    terms = terms.reshape(heads * dk // 128, 128)
    out, right = pl.pallas_call(
        functools.partial(suffix_kernel, count, rows),
        out_shape=(
            jax.ShapeDtypeStruct((count, rows, dv), jnp.float32),
            jax.ShapeDtypeStruct(terms.shape, jnp.float32),
        ),
        in_specs=[vmem] * 3,
        out_specs=(vmem, vmem),
        scratch_shapes=[
            pltpu.VMEM((count, 2, rows, dv), jnp.float32),
            pltpu.VMEM((count, rows, dv), jnp.float32),
            pltpu.VMEM((count,) + terms.shape, jnp.float32),
            dma((2,)),
            dma((count,)),
            dma((count,)),
            dma((count,)),
            dma((count,)),
            dma((count,)),
            dma((count,)),
        ],
        compiler_params=pltpu.CompilerParams(collective_id=1, has_side_effects=True),
        name="suffix_states",
    )(packed, reach_sum.reshape(count, rows, dv), terms)
    return out.reshape(local_sum.shape), right.reshape(1, -1)


def return_kernel(
    experts, width, steps, parts, tokens, grads, hidden, d_gate, d_up, mixer,
    returned, mixer_all, gate_out, up_out, down_out,
    core_held, pair_stage, pair_held, send_stage, gate_stage, up_stage, down_stage,
    out_sem, local_sem, core_send, core_recv, pair_send, pair_recv, back_send, back_recv,
    mix_send, mix_recv, over_send, over_recv,
):
    e, p, t = lax.axis_index("ep"), lax.axis_index("pair"), lax.axis_index("tp")
    barrier = pltpu.get_barrier_semaphore()
    for k in range(1, experts):
        pl.semaphore_signal(
            barrier, inc=1, device_id=(lax.rem(e + k, experts), p, t), device_id_type=MESH
        )
    pl.semaphore_signal(barrier, inc=1, device_id=(e, 1 - p, t), device_id_type=MESH)
    pl.semaphore_signal(barrier, inc=1, device_id=(e, p, 1 - t), device_id_type=MESH)
    pl.semaphore_wait(barrier, experts + 1)
    own_columns = pl.ds(pl.multiple_of(t * width, 128), width)
    core_columns = pl.ds(pl.multiple_of((1 - t) * width, 128), width)

    def owner(k):
        return lax.rem(e + 1 + k, experts)

    def core_copy(which, k):
        side = 1 - p if which == 0 else p
        return pltpu.make_async_remote_copy(
            src_ref=parts.at[side, owner(k), :, core_columns],
            dst_ref=core_held.at[which, k],
            send_sem=core_send.at[which, k],
            recv_sem=core_recv.at[which, k],
            device_id=(e, p, 1 - t),
            device_id_type=MESH,
        )

    def pair_copy(k):
        return pltpu.make_async_remote_copy(
            src_ref=pair_stage.at[k], dst_ref=pair_held.at[k], send_sem=pair_send.at[k],
            recv_sem=pair_recv.at[k], device_id=(e, 1 - p, t), device_id_type=MESH,
        )

    def back_copy(k):
        return pltpu.make_async_remote_copy(
            src_ref=send_stage.at[k], dst_ref=returned.at[e], send_sem=back_send.at[k],
            recv_sem=back_recv.at[k], device_id=(owner(k), p, t), device_id_type=MESH,
        )

    def mix_copy(k):
        return pltpu.make_async_remote_copy(
            src_ref=mixer, dst_ref=mixer_all.at[e, p], send_sem=mix_send.at[k],
            recv_sem=mix_recv.at[k], device_id=(owner(k), p, t), device_id_type=MESH,
        )

    def from_owner(k):
        return lax.rem(e - 1 - k + 2 * experts, experts)

    def mix_landed(k):
        place = mixer_all.at[from_owner(k), p]
        return pltpu.make_async_remote_copy(
            src_ref=place, dst_ref=place, send_sem=mix_send.at[k], recv_sem=mix_recv.at[k],
            device_id=(from_owner(k), p, t), device_id_type=MESH,
        )

    def over_copy(k, side):
        place = mixer_all.at[from_owner(k), side]
        return pltpu.make_async_remote_copy(
            src_ref=place, dst_ref=place, send_sem=over_send.at[k], recv_sem=over_recv.at[k],
            device_id=(e, 1 - p, t), device_id_type=MESH,
        )

    mix_own = pltpu.make_async_copy(mixer, mixer_all.at[e, p], mix_recv.at[experts - 1])
    mix_own.start()

    def half_of(which, k):
        side = 1 - p if which == 0 else p
        mine = parts[side, owner(k), :, own_columns].astype(jnp.float32)
        return (mine + core_held[which, k].astype(jnp.float32)).astype(jnp.bfloat16)

    for which in range(2):
        for k in range(experts):
            core_copy(which, k).start()
    for k in range(experts):
        core_copy(0, k).wait_recv()
        pair_stage[k] = half_of(0, k)
        if k:
            pair_copy(k - 1).start()
    pair_copy(experts - 1).start()
    for k in range(experts - 1):
        mix_copy(k).start()
    for k in range(experts):
        core_copy(1, k).wait_recv()

    def down_step(i, carry):
        cut = pl.ds(pl.multiple_of(i * 128, 128), 128)
        down_stage[cut, :] = lax.dot_general(
            hidden[:, cut], grads[...], DOWNWARD, preferred_element_type=jnp.float32
        ).astype(jnp.bfloat16)
        pltpu.make_async_copy(down_stage.at[cut], down_out.at[cut], out_sem.at[0]).start()
        return carry

    lax.fori_loop(0, hidden.shape[1] // 128, down_step, 0)
    span = tokens.shape[1] // steps
    each = experts // steps

    def weight_step(i, carry):
        cut = pl.ds(pl.multiple_of(i * span, span), span)
        gate_stage[cut, :] = lax.dot_general(
            tokens[:, cut], d_gate[...], DOWNWARD, preferred_element_type=jnp.float32
        ).astype(jnp.bfloat16)
        for j in range(each):
            k = i * each + j
            pair_copy(k).wait_recv()
            total = half_of(1, k).astype(jnp.float32) + pair_held[k].astype(jnp.float32)
            send_stage[k] = total.astype(jnp.bfloat16)
        up_stage[cut, :] = lax.dot_general(
            tokens[:, cut], d_up[...], DOWNWARD, preferred_element_type=jnp.float32
        ).astype(jnp.bfloat16)
        for j in range(each):
            k = i * each + j

            @pl.when(k < experts - 1)
            def _():
                back_copy(k).start()

        for j in range(each):
            k = i * each + j

            @pl.when(k < experts - 1)
            def _():
                mix_landed(k).wait_recv()
                over_copy(k, p).start()

        pltpu.make_async_copy(gate_stage.at[cut], gate_out.at[cut], out_sem.at[1]).start()
        pltpu.make_async_copy(up_stage.at[cut], up_out.at[cut], out_sem.at[2]).start()
        return carry

    lax.fori_loop(0, steps, weight_step, 0)
    own = pltpu.make_async_copy(send_stage.at[experts - 1], returned.at[e], local_sem)
    own.start()
    own.wait()
    mix_own.wait()
    over_copy(experts - 1, p).start()
    for k in range(experts - 1):
        source = lax.rem(e - 1 - k + experts, experts)
        pltpu.make_async_remote_copy(
            src_ref=returned.at[source], dst_ref=returned.at[source], send_sem=back_send.at[k],
            recv_sem=back_recv.at[k], device_id=(source, p, t), device_id_type=MESH,
        ).wait_recv()
    for k in range(experts):
        core_copy(0, k).wait_send()
        core_copy(1, k).wait_send()
        pair_copy(k).wait_send()
        over_copy(k, 1 - p).wait_recv()
        over_copy(k, p).wait_send()
        if k < experts - 1:
            back_copy(k).wait_send()
            mix_copy(k).wait_send()
    pltpu.make_async_copy(down_stage, down_out, out_sem.at[0]).wait()
    pltpu.make_async_copy(gate_stage, gate_out, out_sem.at[1]).wait()
    pltpu.make_async_copy(up_stage, up_out, out_sem.at[2]).wait()


def return_rows(parts, tokens, grads, hidden, d_gate, d_up, mixer):
    _, experts, capacity, model_width = parts.shape
    width = model_width // 2
    units = hidden.shape[1]
    half = (experts, capacity, width)
    vmem = pl.BlockSpec(memory_space=pltpu.VMEM)
    hbm = pl.BlockSpec(memory_space=pl.ANY)
    dma = pltpu.SemaphoreType.DMA
    wide, tall = (model_width, units), (units, model_width)
    kind = jnp.bfloat16
    shape = jax.ShapeDtypeStruct
    return pl.pallas_call(
        functools.partial(return_kernel, experts, width, min(8, experts)),
        out_shape=(shape(half, kind), shape((experts, 2) + mixer.shape, kind), shape(wide, kind), shape(wide, kind), shape(tall, kind)),
        in_specs=[vmem] * 7,
        out_specs=(vmem, vmem, hbm, hbm, hbm),
        scratch_shapes=[
            pltpu.VMEM((2,) + half, kind),
            pltpu.VMEM(half, kind),
            pltpu.VMEM(half, kind),
            pltpu.VMEM(half, kind),
            pltpu.VMEM(wide, kind),
            pltpu.VMEM(wide, kind),
            pltpu.VMEM(tall, kind),
            dma((3,)),
            dma,
            dma((2, experts)),
            dma((2, experts)),
            dma((experts,)),
            dma((experts,)),
            dma((experts,)),
            dma((experts,)),
            dma((experts,)),
            dma((experts,)),
            dma((experts,)),
            dma((experts,)),
        ],
        compiler_params=pltpu.CompilerParams(
            collective_id=2, has_side_effects=True, vmem_limit_bytes=60 * 1024 * 1024
        ),
        name="return_rows",
    )(parts, tokens, grads, hidden, d_gate, d_up, mixer)


def block_back(carried, inputs):
    q_block, k_block, v_block, o_block, decay_block, state_in = inputs
    cumul = jnp.cumsum(decay_block, axis=0)
    block_total = cumul[-1]
    growth = jnp.exp(cumul)
    shrink = jnp.exp(-cumul)
    to_end = jnp.exp(block_total[None] - cumul)
    span_len = q_block.shape[0]
    causal = (jnp.arange(span_len)[:, None] >= jnp.arange(span_len)[None, :]).astype(jnp.float32)
    q_grow = q_block * growth
    k_shrink = k_block * shrink
    scores = jnp.einsum("thv,shv->hts", o_block, v_block, precision=PRECISE) * causal
    mutual = jnp.einsum("thd,shd->hts", q_grow, k_shrink, precision=PRECISE) * causal
    grad_q = growth * (
        jnp.einsum("thv,hdv->thd", o_block, state_in, precision=PRECISE)
        + jnp.einsum("hts,shd->thd", scores, k_shrink, precision=PRECISE)
    )
    grad_k = to_end * jnp.einsum(
        "hdv,shv->shd", carried, v_block, precision=PRECISE
    ) + shrink * jnp.einsum("hts,thd->shd", scores, q_grow, precision=PRECISE)
    grad_v = jnp.einsum("shd,hdv->shv", k_block * to_end, carried, precision=PRECISE) + jnp.einsum(
        "hts,thv->shv", mutual, o_block, precision=PRECISE
    )
    contrib = q_block * grad_q - k_block * grad_k
    carried = jnp.exp(block_total)[:, :, None] * carried + jnp.einsum(
        "thd,thv->hdv", q_grow, o_block, precision=PRECISE
    )
    return (carried, (grad_q, grad_k, grad_v, contrib))


def body(
    moe_input,
    out_grad,
    route_ids,
    route_weights,
    gate_w,
    up_w,
    down_w,
    mixer_out,
    out_weight,
    queries,
    keys,
    values,
    log_decay,
    block_states,
):
    sp_count = sp_size()
    experts = lax.axis_size("ep")
    tok_rows = moe_input.shape[0]
    model_width = moe_input.shape[1]
    capacity = 3 * tok_rows // experts
    flat_ids = route_ids.reshape(-1)
    one_hot = (flat_ids[:, None] == jnp.arange(experts, dtype=jnp.int32)[None, :]).astype(jnp.int32)
    earlier_count = jnp.sum(jnp.cumsum(one_hot, axis=0) * one_hot, axis=1) - 1
    slot_index = flat_ids * capacity + earlier_count
    dispatch = (
        jnp.arange(experts * capacity, dtype=jnp.int32)[:, None] == slot_index[None, :]
    ).astype(jnp.bfloat16)
    token_pick = jnp.sum(dispatch.reshape(experts * capacity, tok_rows, 2), axis=2)
    col_count = model_width // lax.axis_size("tp")
    col_start = lax.axis_index("tp") * col_count
    source_tokens = lax.dynamic_slice_in_dim(moe_input, col_start, col_count, 1)
    source_grads = lax.dynamic_slice_in_dim(out_grad, col_start, col_count, 1)
    send_width = source_tokens.shape[1]
    scaled = (route_weights[:, :, None] * source_grads[:, None, :].astype(jnp.float32)).astype(
        jnp.bfloat16
    )
    scaled = scaled.reshape(2 * tok_rows, send_width)
    token_send = jnp.dot(token_pick, source_tokens, preferred_element_type=jnp.float32).astype(
        jnp.bfloat16
    )
    grad_send = jnp.dot(dispatch, scaled, preferred_element_type=jnp.float32).astype(jnp.bfloat16)

    arrived_tokens, arrived_grads = dispatch_rows(
        token_send.reshape(experts, capacity, send_width),
        grad_send.reshape(experts, capacity, send_width),
    )
    arrived_tokens = arrived_tokens.reshape(sp_count * capacity, model_width)
    arrived_grads = arrived_grads.reshape(sp_count * capacity, model_width)
    gate_mat = gate_w[0]
    up_mat = up_w[0]
    down_mat = down_w[0]
    gate_pre = jnp.dot(arrived_tokens, gate_mat, preferred_element_type=jnp.float32)
    up_pre = jnp.dot(arrived_tokens, up_mat, preferred_element_type=jnp.float32)
    sigmoid_gate = jax.nn.sigmoid(gate_pre)
    hidden = (gate_pre * sigmoid_gate * up_pre).astype(jnp.bfloat16)
    d_hidden = lax.dot_general(arrived_grads, down_mat, ACROSS, preferred_element_type=jnp.float32)
    d_up = (d_hidden * gate_pre * sigmoid_gate).astype(jnp.bfloat16)
    d_gate = (d_hidden * up_pre * sigmoid_gate * (1.0 + gate_pre * (1.0 - sigmoid_gate))).astype(
        jnp.bfloat16
    )
    partial_value = lax.dot_general(
        d_gate, gate_mat, ACROSS, preferred_element_type=jnp.float32
    ) + lax.dot_general(d_up, up_mat, ACROSS, preferred_element_type=jnp.float32)
    parts = partial_value.astype(jnp.bfloat16)
    returned, mixer_all, grad_gate, grad_up, grad_down = return_rows(
        parts.reshape(2, experts, capacity, model_width),
        arrived_tokens,
        arrived_grads,
        hidden,
        d_gate,
        d_up,
        mixer_out,
    )
    returned = returned.reshape(experts * capacity, col_count)
    moe_grad = lax.dot_general(token_pick, returned, DOWNWARD, preferred_element_type=jnp.float32)
    grad_mid = (source_grads.astype(jnp.float32) + moe_grad).astype(jnp.bfloat16)
    grad_mid = lax.all_gather(grad_mid, "tp", axis=1, tiled=True)
    mixer_all = mixer_all.reshape(sp_count * tok_rows, -1)
    mid_columns = lax.all_to_all(grad_mid, SP, split_axis=1, concat_axis=0, tiled=True)
    grad_out_weight = lax.dot_general(
        mixer_all, mid_columns, DOWNWARD, preferred_element_type=jnp.float32
    )
    grad_mixed = lax.dot_general(
        grad_mid, out_weight, ACROSS, preferred_element_type=jnp.float32
    ).astype(jnp.bfloat16)
    heads_local = queries.shape[1] // DK
    blocks = tok_rows // BLK

    def shaped(array, depth):
        return array.astype(jnp.float32).reshape(blocks, BLK, heads_local, depth)

    q_blocks = shaped(queries, DK)
    k_blocks = shaped(keys, DK)
    v_blocks = shaped(values, DV)
    decay_blocks = shaped(log_decay, DK)
    inputs = (q_blocks, k_blocks, v_blocks, shaped(grad_mixed, DV), decay_blocks, block_states)
    zero_state = jnp.zeros((heads_local, DK, DV), jnp.float32)
    local_sum, (grad_q, grad_k, grad_v, contrib) = lax.scan(
        block_back, zero_state, inputs, reverse=True, unroll=True
    )
    cumul = jnp.cumsum(decay_blocks, axis=1)
    totals = cumul[:, -1]
    offsets = jnp.cumsum(totals, axis=0) - totals
    position = cumul + offsets[:, None]
    device_total = jnp.sum(totals, axis=0)
    fade_out = jnp.exp(device_total[None, None] - position)
    k_fade = k_blocks * fade_out
    reach_sum = jnp.einsum("nshd,nshv->hdv", k_fade, v_blocks, precision=PRECISE)
    from_right, right_terms = suffix_states(
        jnp.exp(device_total), local_sum, reach_sum, jnp.sum(contrib, axis=(0, 1))
    )
    key_part = jnp.einsum("nshv,hdv->nshd", v_blocks, from_right, precision=PRECISE)
    grad_k = grad_k + fade_out * key_part
    grad_v = grad_v + jnp.einsum("nshd,hdv->nshv", k_fade, from_right, precision=PRECISE)
    contrib = (contrib - k_fade * key_part).reshape(tok_rows, heads_local * DK)
    grad_decay = jnp.flip(jnp.cumsum(jnp.flip(contrib, 0), axis=0), 0) + right_terms
    return (
        grad_q.reshape(tok_rows, heads_local * DK).astype(jnp.bfloat16),
        grad_k.reshape(tok_rows, heads_local * DK).astype(jnp.bfloat16),
        grad_v.reshape(tok_rows, heads_local * DV).astype(jnp.bfloat16),
        grad_decay,
        grad_out_weight,
        grad_gate[None],
        grad_up[None],
        grad_down[None],
    )


def solution(mesh):
    sp_count, tp_count = mesh.devices.shape
    mesh = Mesh(mesh.devices.reshape(sp_count // 2, 2, tp_count), ("ep", "pair", "tp"))
    placed = (
        P(SP, None),
        P(SP, None),
        P(SP, None),
        P(SP, None),
        P(SP, None, "tp"),
        P(SP, None, "tp"),
        P(SP, "tp", None),
        P(SP, "tp"),
        P("tp", None),
        P(SP, "tp"),
        P(SP, "tp"),
        P(SP, "tp"),
        P(SP, "tp"),
        P(SP, "tp", None, None),
    )
    return jax.shard_map(
        body,
        mesh=mesh,
        in_specs=placed,
        out_specs=(
            P(SP, "tp"),
            P(SP, "tp"),
            P(SP, "tp"),
            P(SP, "tp"),
            P("tp", SP),
            P(SP, None, "tp"),
            P(SP, None, "tp"),
            P(SP, "tp", None),
        ),
        check_vma=False,
    )
```
